32 devices in a mesh: ep: 8 (over z, y), tp: 4 (over x, core).
Axes of the slice: x: 2, y: 2, z: 4, core: 2. Of those that a mesh axis runs over, the one named last changes fastest.
Arguments:
- queries: bfloat16 [4096, 1024], P('ep', 'tp'), may hold values from -6 to 6
- keys: bfloat16 [4096, 512], P('ep', 'tp'), may hold values from -6 to 6
- values: bfloat16 [4096, 512], P('ep', 'tp'), may hold values from -6 to 6
- forget_cache: float32 [8, 4096], P('tp'), may hold values from -412 to 0, as said below
- query_gain: float32 [128], replicated, may hold values from 0.6 to 6
- key_gain: float32 [128], replicated, may hold values from 0.6 to 6
- mixer_out: bfloat16 [1024, 2048], replicated, may hold values from -0.75 to 0.75
- expert_input: bfloat16 [4096, 2048], P(('ep', 'tp')), may hold values from -6 to 6
- norm_gain: float32 [2048], replicated, may hold values from 0.1 to 1.9
- routes: int32 [4096, 2], P(('ep', 'tp')), may hold values from 0 to 31, all different within a row; in each aligned block of 128 rows (0 to 127, 128 to 255, ...) at most 16 rows name the same one
- route_weights: float32 [4096, 2], P(('ep', 'tp')), may hold values from 0.1 to 1
- w_gate: bfloat16 [32, 2048, 1024], P('ep', None, 'tp'), may hold values from -0.125 to 0.125
- w_up: bfloat16 [32, 2048, 1024], P('ep', None, 'tp'), may hold values from -0.125 to 0.125
- w_down: bfloat16 [32, 2048, 1024], P('ep', None, 'tp'), may hold values from -0.1875 to 0.1875
Outputs:
- mixed: bfloat16 [4096, 2048], P(('ep', 'tp'))
- routed: bfloat16 [4096, 2048], P(('ep', 'tp'))
The draws below stay inside these ranges and needn't reach their ends.
Inputs may be any that keep to these rules, and one draw needn't show every extreme that they name: `routes`: each row names 2 different experts; among the rows of one device no expert is named by more than 16 rows, a bound that some block reaches. `forget_cache`: never rises along the positions.
All inputs are finite; a program needn't handle non-finite values.
Results may differ from the reference program's by a relative error of at most 0.013.
The reference program's roundings to bfloat16 on the way count: a program that leaves them out, or rounds other values in their place, can miss the bound.
Values may be sent and summed in bfloat16 or wider, within the bound.
A program may use at most 128 MiB of HBM per device.

```python
import math
import jax
import jax.numpy as jnp
import numpy as np
from jax import lax

D = 2048
QUERY_HEADS = 8
KV_HEADS = 4
HD = 128
EXPERTS = 32
TOPK = 2
FF = 1024
TB_DEV = 128
CAP = 16
ATTENTION_TOKENS = 4096
TOK_B = 4096
N_EP = 8
N_TP = 4


def draw_forget_cache(key, part):
    parallel_flows = jax.random.split(jax.random.fold_in(key, 11), 5)
    token_positions = jnp.arange(ATTENTION_TOKENS, dtype=jnp.int32)
    order = jax.random.permutation(parallel_flows[0], QUERY_HEADS)
    quick = order < QUERY_HEADS // 2
    rate = jnp.where(quick, 1.0 / 40.0, 0.8 / ATTENTION_TOKENS)
    rough = jax.random.uniform(parallel_flows[1], (QUERY_HEADS, ATTENTION_TOKENS), jnp.float32, 0.3, 1.7)
    blocks = 16
    factor = jnp.exp(jax.random.uniform(parallel_flows[2], (QUERY_HEADS, blocks), jnp.float32, -0.7, 0.7))
    which = token_positions * blocks // ATTENTION_TOKENS
    steps = -rate[:, None] * rough * factor[:, which]
    token_groups = jax.random.randint(parallel_flows[3], (QUERY_HEADS, 3), 0, ATTENTION_TOKENS)
    depth = jnp.log(jax.random.uniform(parallel_flows[4], (QUERY_HEADS, 3), jnp.float32, 0.5, 0.8))
    masked_scores = token_positions[None, None, :] == token_groups[:, :, None]
    steps = steps + jnp.sum(jnp.where(masked_scores, depth[:, :, None], 0.0), axis=1)
    return jnp.cumsum(steps, axis=1).astype(jnp.float32)


def draw_query_gain(key, part):
    return jax.random.uniform(jax.random.fold_in(key, 21), (HD,), jnp.float32, 0.6, 1.4)


def draw_key_gain(key, part):
    return jax.random.uniform(jax.random.fold_in(key, 31), (HD,), jnp.float32, 0.6, 1.4)


def block_scale(own_key, shape, cuts, low, largest):
    factor_of = 1.0
    for position, blocks in cuts:
        steps = jax.random.uniform(jax.random.fold_in(jax.random.fold_in(own_key, 6), position), (blocks,), jnp.float32, low / len(cuts), largest / len(cuts))
        factor_of = factor_of * jnp.repeat(jnp.exp(steps), shape[position] // blocks).reshape((-1,) + (1,) * (len(shape) - 1 - position))
    return factor_of


def routed_block(key, own, number, rows, amount, top, most, lean):
    ranking = jax.random.permutation(key, amount)
    crowded, usual = portions_of(amount, rows * top, most, lean, True), portions_of(amount, rows * top, most, lean, False)
    places = jnp.arange(amount)

    def named(tallies, rotation):
        used = int((tallies > 0).sum())
        fixed = max(1, used // 4)
        passed = fixed + (places - fixed + rotation * (used - fixed)) % max(1, amount - fixed)
        return jnp.zeros((amount,), jnp.int32).at[ranking[jnp.where(places < fixed, places, passed)]].set(jnp.asarray(tallies, jnp.int32))

    tallies = jnp.where(number % 4 == 0, named(crowded, number // 4), named(usual, number - number // 4 - 1))
    mixed = jax.random.permutation(jax.random.fold_in(own, 3), amount)
    giver, sink = mixed[0:amount // 2 * 2:2], mixed[1:amount // 2 * 2:2]
    margin = jnp.minimum(tallies[giver] - 1, most - tallies[sink]) // 2
    margin = jnp.where((giver == ranking[0]) | (sink == ranking[0]) | (tallies[sink] == 0), 0, jnp.maximum(margin, 0))
    passed = jax.random.randint(jax.random.fold_in(own, 4), (amount // 2,), 0, 1 << 20) % (margin + 1)
    tallies = tallies.at[giver].add(-passed).at[sink].add(passed)
    items = jnp.searchsorted(jnp.cumsum(tallies), jnp.arange(rows * top), side="right").astype(jnp.int32)
    grid = items.reshape(top, rows).T
    grid = grid[jax.random.permutation(jax.random.fold_in(own, 1), rows)]
    rotation = jax.random.randint(jax.random.fold_in(own, 2), (rows, 1), 0, top)
    return jnp.take_along_axis(grid, (jnp.arange(top)[None, :] + rotation) % top, axis=1)


def portions_of(number_of, total, limit, slope, full):
    loads = [(1 << 20) // math.isqrt(rank ** slope) + 1 for rank in range(1, number_of + 1)]
    largest = limit if full else min(limit, max(-(-total // number_of), total * loads[0] // sum(loads)))
    least = 1 if total - largest >= number_of - 1 else 0
    holding, spare = [largest] + [least] * (number_of - 1), total - largest - least * (number_of - 1)
    while spare > 0:
        free = [i for i in range(1, number_of) if holding[i] < largest] or [i for i in range(1, number_of) if holding[i] < limit]
        pool, left = sum([loads[i] for i in free]), spare
        for i in free:
            addition = min(limit - holding[i], max(1, left * loads[i] // pool), spare)
            holding[i] = holding[i] + addition
            spare = spare - addition
    return np.array(holding)


def scatter_about(rng, shape, deviation, limit, pieces=(), kind=jnp.bfloat16):
    drawn = deviation * jax.random.normal(rng, shape, jnp.float32)
    if pieces:
        drawn = drawn * block_scale(rng, shape, pieces, -0.22, 0.18)
    return jnp.clip(drawn, -limit, limit).astype(kind)


def setup_inputs(seed: int = 0) -> dict:
    streams_of = jax.random.split(jax.random.key(seed), 15)
    queries = scatter_about(streams_of[0], (ATTENTION_TOKENS, QUERY_HEADS * HD), 1.0, 6.0, ((0, 8), (1, 4)))
    keys = scatter_about(streams_of[1], (ATTENTION_TOKENS, KV_HEADS * HD), 1.0, 6.0, ((0, 8), (1, 4)))
    values = scatter_about(streams_of[2], (ATTENTION_TOKENS, KV_HEADS * HD), 1.0, 6.0, ((0, 8), (1, 4)))
    forget_cache = draw_forget_cache(jax.random.fold_in(streams_of[14], 71), 0)
    query_gain = draw_query_gain(jax.random.fold_in(streams_of[14], 71), 0)
    key_gain = draw_key_gain(jax.random.fold_in(streams_of[14], 71), 0)
    mixer_out = scatter_about(streams_of[6], (QUERY_HEADS * HD, D), (QUERY_HEADS * HD // 16) ** -0.5, 0.75)
    expert_input = scatter_about(streams_of[7], (TOK_B, D), 1.0, 6.0, ((0, 32),))
    norm_gain = jnp.clip(1.0 + 0.18 * jax.random.normal(streams_of[8], (D,), jnp.float32), 0.1, 1.9)
    routes_keys = jax.random.split(jax.random.fold_in(streams_of[9], 1), TOK_B // TB_DEV)
    routes_turns = jax.random.permutation(jax.random.fold_in(streams_of[9], 3), TOK_B // TB_DEV)
    routes = jax.vmap(lambda own, number: routed_block(jax.random.fold_in(streams_of[9], 2), own, number, TB_DEV, EXPERTS, TOPK, CAP, 1))(routes_keys, routes_turns).reshape((TOK_B, TOPK))
    route_weights = jnp.clip(0.1 + 0.9 * jax.random.uniform(streams_of[10], (TOK_B, TOPK), jnp.float32) ** block_scale(streams_of[10], (TOK_B, TOPK), ((0, 32),), -0.2, 0.2), 0.1, 1.0)
    w_gate = scatter_about(streams_of[11], (EXPERTS, D, FF), D ** -0.5, 0.125, ((0, 8), (2, 4)))
    w_up = scatter_about(streams_of[12], (EXPERTS, D, FF), D ** -0.5, 0.125, ((0, 8), (2, 4)))
    w_down = scatter_about(streams_of[13], (EXPERTS, D, FF), FF ** -0.5, 0.1875, ((0, 8), (2, 4)))
    return dict(queries=queries, keys=keys, values=values, forget_cache=forget_cache, query_gain=query_gain, key_gain=key_gain, mixer_out=mixer_out, expert_input=expert_input, norm_gain=norm_gain, routes=routes, route_weights=route_weights, w_gate=w_gate, w_up=w_up, w_down=w_down)


EPSILON = 1e-06
NEGATIVE = -1e+30

def rms_scale(inputs, gain):
    inputs = inputs.astype(jnp.float32)
    return inputs * lax.rsqrt(lax.optimization_barrier(jnp.mean(inputs * inputs, axis=-1, keepdims=True)) + EPSILON) * gain

def reference(queries, keys, values, forget_cache, query_gain, key_gain, mixer_out, expert_input, norm_gain, routes, route_weights, w_gate, w_up, w_down):
    total = queries.shape[0]
    group = QUERY_HEADS // KV_HEADS
    normed_q = rms_scale(queries.reshape(total, QUERY_HEADS, HD), query_gain).astype(jnp.bfloat16)
    normed_q = lax.optimization_barrier(normed_q).astype(jnp.float32)
    normed_k = rms_scale(keys.reshape(total, KV_HEADS, HD), key_gain).astype(jnp.bfloat16)
    normed_k = lax.optimization_barrier(normed_k).astype(jnp.float32)
    key_heads = jnp.repeat(normed_k, group, axis=1)
    value_heads = jnp.repeat(values.reshape(total, KV_HEADS, HD).astype(jnp.float32), group, axis=1)
    block = math.gcd(total, 512)
    token_positions = jnp.arange(total, dtype=jnp.int32)
    scale = HD ** (-0.5)

    def one_block(number):
        first = (number * block).astype(jnp.int32)
        query_block = lax.dynamic_slice_in_dim(normed_q, first, block, 0)
        scores = jnp.einsum('qhd,khd->hqk', query_block, key_heads) * scale
        gates_q = lax.dynamic_slice_in_dim(forget_cache, first, block, 1)
        scores = scores + gates_q[:, :, None] - forget_cache[:, None, :]
        allowed = token_positions[None, :] <= (first + jnp.arange(block, dtype=jnp.int32))[:, None]
        scores = jnp.where(allowed[None], scores, NEGATIVE)
        highest = lax.optimization_barrier(jnp.max(scores, axis=2, keepdims=True))
        weights = jnp.where(allowed[None], jnp.exp(scores - highest), 0.0)
        denom = lax.optimization_barrier(jnp.sum(weights, axis=2))
        rounded = lax.optimization_barrier(weights.astype(jnp.bfloat16)).astype(jnp.float32)
        numer = jnp.einsum('hqk,khd->qhd', rounded, value_heads)
        return (numer / denom.T[:, :, None]).astype(jnp.bfloat16)
    attended = lax.map(one_block, jnp.arange(total // block, dtype=jnp.int32)).reshape(total, QUERY_HEADS * HD)
    mixed = jnp.dot(attended, mixer_out, preferred_element_type=jnp.float32).astype(jnp.bfloat16)
    normed_b = rms_scale(expert_input, norm_gain).astype(jnp.bfloat16)
    count = expert_input.shape[0]
    flat = routes.reshape(-1)
    most = N_EP * N_TP * CAP
    padded = jnp.concatenate([normed_b, jnp.zeros((1, D), jnp.bfloat16)], axis=0)
    flat_weights = jnp.concatenate([route_weights.reshape(-1), jnp.zeros((1,), jnp.float32)])

    def per_expert(totals, expert):
        chosen = jnp.nonzero(flat == expert, size=most, fill_value=flat.shape[0])[0].astype(jnp.int32)
        owner = (chosen // TOPK).astype(jnp.int32)
        rows = padded[owner]
        gate = jnp.dot(rows, w_gate[expert], preferred_element_type=jnp.float32)
        upward = jnp.dot(rows, w_up[expert], preferred_element_type=jnp.float32)
        hidden = (jax.nn.silu(gate) * upward).astype(jnp.bfloat16)
        output = jnp.dot(hidden, w_down[expert].T, preferred_element_type=jnp.float32).astype(jnp.bfloat16)
        return (totals.at[owner].add(output.astype(jnp.float32) * flat_weights[chosen][:, None]), None)
    totals = lax.scan(per_expert, jnp.zeros((count + 1, D), jnp.float32), jnp.arange(EXPERTS, dtype=jnp.int32))[0]
    routed = totals[:count].astype(jnp.bfloat16)
    return (mixed, routed)
```

```python
import functools

import jax
import jax.numpy as jnp
from jax import lax
from jax.experimental import pallas as pl
from jax.experimental.pallas import tpu as pltpu
from jax.sharding import PartitionSpec as P

CAP = 16
EPSILON = 1e-06
NEGATIVE = -1e30
MESH = pl.DeviceIdType.MESH
VMEM_LIMIT = 62 * 1024 * 1024


def rms_scale(inputs, gain):
    inputs = inputs.astype(jnp.float32)
    return inputs * lax.rsqrt(jnp.mean(inputs * inputs, axis=-1, keepdims=True) + EPSILON) * gain


def places(n_tp):
    ep, tp = lax.axis_index("ep"), lax.axis_index("tp")
    core = tp + 1 - 2 * lax.rem(tp, 2)
    across = lax.rem(tp + n_tp // 2, n_tp)
    corner = lax.rem(core + n_tp // 2, n_tp)
    return ep, tp, core, across, corner


def meet(n_ep, n_tp):
    ep, tp = lax.axis_index("ep"), lax.axis_index("tp")
    barrier = pltpu.get_barrier_semaphore()
    for step in range(1, n_ep):
        pl.semaphore_signal(
            barrier, inc=1, device_id=(lax.rem(ep + step, n_ep), tp), device_id_type=MESH
        )
    for step in range(1, n_tp):
        pl.semaphore_signal(
            barrier, inc=1, device_id=(ep, lax.rem(tp + step, n_tp)), device_id_type=MESH
        )
    pl.semaphore_wait(barrier, n_ep + n_tp - 2)


def remote(src, dst, send, recv, ep, tp):
    return pltpu.make_async_remote_copy(
        src_ref=src, dst_ref=dst, send_sem=send, recv_sem=recv, device_id=(ep, tp), device_id_type=MESH
    )


def gather_kernel(
    n_ep,
    n_tp,
    heads,
    outg,
    kv,
    q,
    fq,
    fk,
    pieces,
    att_all,
    kvbuf,
    att,
    high,
    denom,
    accum,
    a_send,
    a_recv,
    x_send,
    x_recv,
    c_send,
    c_recv,
    d_send,
    d_recv,
    k_send,
    k_recv,
    t_send,
    t_recv,
    own_sem,
):
    ep, tp, core, across, corner = places(n_tp)
    rows, head_dim = kv.shape[0], q.shape[1]
    part = rows // n_tp
    scale = head_dim ** (-0.5)
    meet(n_ep, n_tp)

    def kv_copy(source, step):
        return remote(kv, kvbuf.at[source], k_send.at[step], k_recv.at[source], lax.rem(ep + step, n_ep), tp)

    def a_copy(source, step):
        dest = lax.rem(ep + step, n_ep)
        return remote(outg.at[dest], pieces.at[tp, source], a_send.at[step], a_recv.at[source], dest, tp)

    def x_copy(src, owner, source):
        return remote(src, pieces.at[owner, source], x_send.at[source], x_recv.at[source], ep, across)

    def c_copy(src, owner, source):
        return remote(src, pieces.at[owner, source], c_send.at[source], c_recv.at[source], ep, core)

    def d_copy(src, owner, source):
        return remote(src, pieces.at[owner, source], d_send.at[source], d_recv.at[source], ep, core)

    def start_kv(step, carry):
        @pl.when(ep + step < n_ep)
        def _():
            kv_copy(ep, step).start()

        return carry

    lax.fori_loop(1, n_ep, start_kv, 0)
    own = pltpu.make_async_copy(outg.at[ep], pieces.at[tp, ep], own_sem)
    own.start()
    x_copy(outg.at[ep], tp, ep).start()
    c_copy(outg.at[ep], tp, ep).start()

    def start_a(step, carry):
        a_copy(ep, step).start()
        return carry

    lax.fori_loop(1, n_ep, start_a, 0)

    tile = rows // 2

    def block(source, keys_ref, diagonal):
        keys = keys_ref[:, :head_dim]
        vals = keys_ref[:, head_dim:]
        for head in range(heads):
            key_gate = fk[source, head : head + 1, :]
            for half in range(2):
                span = pl.ds(head * rows + half * tile, tile)
                scores = lax.dot_general(
                    q[span, :], keys, (((1,), (1,)), ((), ())), preferred_element_type=jnp.float32
                )
                scores = scores * scale + fq[span, :] - key_gate
                if diagonal:
                    qpos = half * tile + lax.broadcasted_iota(jnp.int32, scores.shape, 0)
                    kpos = lax.broadcasted_iota(jnp.int32, scores.shape, 1)
                    scores = jnp.where(kpos <= qpos, scores, NEGATIVE)
                top = jnp.max(scores, axis=1, keepdims=True)
                if diagonal:
                    newest = top
                else:
                    before = high[span, :]
                    newest = jnp.maximum(before, top)
                weights = jnp.exp(scores - newest)
                total = jnp.sum(weights, axis=1, keepdims=True)
                product = jnp.dot(
                    weights.astype(jnp.bfloat16), vals, preferred_element_type=jnp.float32
                )
                if not diagonal:
                    factor = jnp.exp(before - newest)
                    total = denom[span, :] * factor + total
                    product = accum[span, :] * factor + product
                high[span, :] = newest
                denom[span, :] = total
                accum[span, :] = product

    block(ep, kv, True)

    def relay(source):
        x_copy(outg.at[ep], across, source).wait_recv()
        d_copy(pieces.at[across, source], across, source).start()

    def onward(step, carry):
        source = lax.rem(ep - step + n_ep, n_ep)
        a_copy(source, step).wait_recv()
        x_copy(pieces.at[tp, source], tp, source).start()
        c_copy(pieces.at[tp, source], tp, source).start()

        @pl.when(ep - step >= 0)
        def _():
            kv_copy(source, step).wait_recv()
            block(source, kvbuf.at[source], False)

        relay(lax.rem(source + 1, n_ep))
        return carry

    lax.fori_loop(1, n_ep, onward, 0)

    for head in range(heads):
        span = pl.ds(head * rows, rows)
        result = (accum[span, :] / denom[span, :]).astype(jnp.bfloat16)
        for owner in range(n_tp):
            att[owner, head] = result[owner * part : (owner + 1) * part]
    relay(lax.rem(ep + 1, n_ep))

    def t_copy(source, step):
        dest = lax.rem(tp + step, n_tp)
        return remote(att.at[dest], att_all.at[source], t_send.at[step], t_recv.at[source], ep, dest)

    for step in range(1, n_tp):
        t_copy(tp, step).start()
    att_all[tp] = att[tp]

    def finish(source, carry):
        c_copy(outg.at[ep], core, source).wait()
        d_copy(outg.at[ep], corner, source).wait()
        x_copy(outg.at[ep], tp, source).wait_send()
        return carry

    lax.fori_loop(0, n_ep, finish, 0)

    def sent(step, carry):
        a_copy(ep, step).wait_send()

        @pl.when(ep + step < n_ep)
        def _():
            kv_copy(ep, step).wait_send()

        return carry

    lax.fori_loop(1, n_ep, sent, 0)
    for step in range(1, n_tp):
        t_copy(lax.rem(tp - step + n_tp, n_tp), step).wait()
    own.wait()


def expert_kernel(x, gate_w, up_w, down_w, out):
    blocks, _, cap, width = x.shape
    chunk = min(blocks, 512 // cap)

    def some(number, carry):
        span = pl.ds(number * chunk, chunk)
        rows = x[span, 0].reshape(chunk * cap, width)
        gate = jnp.dot(rows, gate_w[0], preferred_element_type=jnp.float32)
        upward = jnp.dot(rows, up_w[0], preferred_element_type=jnp.float32)
        hidden = (gate / (1.0 + jnp.exp(-gate)) * upward).astype(jnp.bfloat16)
        result = lax.dot_general(
            hidden, down_w[0], (((1,), (1,)), ((), ())), preferred_element_type=jnp.float32
        )
        out[span, 0] = result.astype(jnp.bfloat16).reshape(chunk, cap, width)
        return carry

    lax.fori_loop(0, blocks // chunk, some, 0)


def return_kernel(
    n_ep,
    n_tp,
    part_ref,
    att_all,
    mixer,
    slots,
    route_weights,
    mixed,
    routed,
    near_own,
    near_far,
    sum_x,
    got_x,
    sum_r,
    back,
    n_send,
    n_recv,
    f_send,
    f_recv,
    x_send,
    x_recv,
    r_send,
    r_recv,
):
    ep, tp, core, across, corner = places(n_tp)
    meet(n_ep, n_tp)

    def far_copy(dest):
        return remote(part_ref.at[corner, dest], near_far.at[dest], f_send.at[dest], f_recv.at[dest], ep, core)

    def own_copy(dest):
        return remote(part_ref.at[core, dest], near_own.at[dest], n_send.at[dest], n_recv.at[dest], ep, core)

    def x_copy(dest):
        return remote(sum_x.at[dest], got_x.at[dest], x_send.at[dest], x_recv.at[dest], ep, across)

    def r_copy(source, dest):
        return remote(sum_r.at[dest], back.at[source], r_send.at[dest], r_recv.at[source], dest, tp)

    def order(step):
        return lax.rem(ep + step, n_ep)

    def start_far(step, carry):
        far_copy(order(step)).start()
        return carry

    def start_own(step, carry):
        own_copy(order(step)).start()
        return carry

    lax.fori_loop(1, n_ep + 1, start_far, 0)
    lax.fori_loop(1, n_ep + 1, start_own, 0)

    def first(step, carry):
        dest = order(step)
        far_copy(dest).wait_recv()
        sum_x[dest] = (
            part_ref[across, dest].astype(jnp.float32) + near_far[dest].astype(jnp.float32)
        ).astype(jnp.bfloat16)
        x_copy(dest).start()
        return carry

    lax.fori_loop(1, n_ep + 1, first, 0)

    sources, heads, part, head_dim = att_all.shape
    total = None
    for source in range(sources):
        for head in range(heads):
            number = source * heads + head
            term = jnp.dot(
                att_all[source, head],
                mixer[number * head_dim : (number + 1) * head_dim, :],
                preferred_element_type=jnp.float32,
            )
            total = term if total is None else total + term
    mixed[...] = total.astype(jnp.bfloat16)

    def second(dest):
        own_copy(dest).wait_recv()
        x_copy(dest).wait_recv()
        return (
            part_ref[tp, dest].astype(jnp.float32)
            + near_own[dest].astype(jnp.float32)
            + got_x[dest].astype(jnp.float32)
        ).astype(jnp.bfloat16)

    def send_back(step, carry):
        dest = order(step)
        sum_r[dest] = second(dest)
        r_copy(ep, dest).start()
        return carry

    lax.fori_loop(1, n_ep, send_back, 0)
    back[ep] = second(ep)

    def arrived(step, carry):
        source = lax.rem(ep - step + n_ep, n_ep)
        r_copy(source, order(step)).wait()
        return carry

    lax.fori_loop(1, n_ep, arrived, 0)

    def sent(dest, carry):
        far_copy(dest).wait_send()
        own_copy(dest).wait_send()
        x_copy(dest).wait_send()
        return carry

    lax.fori_loop(0, n_ep, sent, 0)

    _, per, width = back.shape
    rows = back[...].reshape(n_ep * per, width)
    summed = None
    for choice in range(slots.shape[1]):
        lanes = lax.broadcasted_iota(jnp.int32, (slots.shape[0], n_ep * per), 1)
        pick = jnp.where(lanes == slots[:, choice : choice + 1], 1.0, 0.0).astype(jnp.bfloat16)
        found = jnp.dot(pick, rows, preferred_element_type=jnp.float32)
        term = found * route_weights[:, choice : choice + 1]
        summed = term if summed is None else summed + term
    routed[...] = summed.astype(jnp.bfloat16)


def on_device(
    n_ep,
    n_tp,
    queries,
    keys,
    values,
    forget_cache,
    query_gain,
    key_gain,
    mixer_out,
    expert_input,
    norm_gain,
    routes,
    route_weights,
    w_gate,
    w_up,
    w_down,
):
    rows, head_dim = keys.shape
    heads = forget_cache.shape[0]
    ep = lax.axis_index("ep")
    local, width, ff = w_gate.shape
    experts = local * n_ep
    tokens = expert_input.shape[0]
    per = local * CAP
    part = rows // n_tp
    vmem = pl.BlockSpec(memory_space=pltpu.VMEM)
    anywhere = pl.BlockSpec(memory_space=pl.ANY)
    dma = pltpu.SemaphoreType.DMA

    normed_q = rms_scale(queries.reshape(rows, heads, head_dim), query_gain).astype(jnp.bfloat16)
    q = normed_q.transpose(1, 0, 2).reshape(heads * rows, head_dim)
    kv = jnp.concatenate([rms_scale(keys, key_gain).astype(jnp.bfloat16), values], axis=1)
    fq = lax.dynamic_slice_in_dim(forget_cache, ep * rows, rows, 1).reshape(heads * rows, 1)
    fk = forget_cache.reshape(heads, n_ep, rows).transpose(1, 0, 2)

    normed = rms_scale(expert_input, norm_gain).astype(jnp.bfloat16)
    names = jnp.arange(experts, dtype=jnp.int32)
    named = [(routes[:, k : k + 1] == names[None, :]) for k in range(routes.shape[1])]
    anyone = functools.reduce(jnp.logical_or, named).astype(jnp.bfloat16)
    at = jnp.arange(tokens, dtype=jnp.int32)
    earlier = (at[None, :] < at[:, None]).astype(jnp.bfloat16)
    prior = jnp.dot(earlier, anyone, preferred_element_type=jnp.float32)
    ranks = [jnp.sum(jnp.where(mine, prior, 0.0), axis=1).astype(jnp.int32) for mine in named]
    slots = jnp.stack([routes[:, k] * CAP + rank for k, rank in enumerate(ranks)], axis=1)
    line = jnp.arange(experts * CAP, dtype=jnp.int32)[:, None]
    place = functools.reduce(
        jnp.logical_or, [line == slots[:, k][None, :] for k in range(slots.shape[1])]
    ).astype(jnp.bfloat16)
    outg = jnp.dot(place, normed, preferred_element_type=jnp.float32).astype(jnp.bfloat16)
    outg = outg.reshape(n_ep, per, width)

    pieces, att_all = pl.pallas_call(
        functools.partial(gather_kernel, n_ep, n_tp, heads),
        out_shape=(
            jax.ShapeDtypeStruct((n_tp, n_ep, per, width), jnp.bfloat16),
            jax.ShapeDtypeStruct((n_tp, heads, part, head_dim), jnp.bfloat16),
        ),
        in_specs=[vmem] * 5,
        out_specs=(anywhere, vmem),
        scratch_shapes=[
            pltpu.VMEM((n_ep, rows, 2 * head_dim), jnp.bfloat16),
            pltpu.VMEM((n_tp, heads, part, head_dim), jnp.bfloat16),
            pltpu.VMEM((heads * rows, 1), jnp.float32),
            pltpu.VMEM((heads * rows, 1), jnp.float32),
            pltpu.VMEM((heads * rows, head_dim), jnp.float32),
        ]
        + [dma((n_ep,))] * 10
        + [dma((n_tp,))] * 2
        + [dma],
        compiler_params=pltpu.CompilerParams(
            collective_id=0, has_side_effects=True, vmem_limit_bytes=VMEM_LIMIT
        ),
        name="gather",
    )(outg, kv, q, fq, fk)

    blocks = n_tp * n_ep
    row_spec = pl.BlockSpec((blocks, 1, CAP, width), lambda e: (0, e, 0, 0))
    weight_spec = pl.BlockSpec((1, width, ff), lambda e: (e, 0, 0))
    partial_sums = pl.pallas_call(
        expert_kernel,
        out_shape=jax.ShapeDtypeStruct((blocks, local, CAP, width), jnp.bfloat16),
        grid=(local,),
        in_specs=[row_spec, weight_spec, weight_spec, weight_spec],
        out_specs=row_spec,
        compiler_params=pltpu.CompilerParams(vmem_limit_bytes=VMEM_LIMIT),
        name="experts",
    )(pieces.reshape(blocks, local, CAP, width), w_gate, w_up, w_down)
    partial_sums = partial_sums.reshape(n_tp, n_ep, per, width)

    buffer = pltpu.VMEM((n_ep, per, width), jnp.bfloat16)
    return pl.pallas_call(
        functools.partial(return_kernel, n_ep, n_tp),
        out_shape=(
            jax.ShapeDtypeStruct((part, width), jnp.bfloat16),
            jax.ShapeDtypeStruct((tokens, width), jnp.bfloat16),
        ),
        in_specs=[vmem] * 5,
        out_specs=(vmem, vmem),
        scratch_shapes=[buffer] * 6 + [dma((n_ep,))] * 8,
        compiler_params=pltpu.CompilerParams(
            collective_id=1, has_side_effects=True, vmem_limit_bytes=VMEM_LIMIT
        ),
        name="give_back",
    )(partial_sums, att_all, mixer_out, slots, route_weights)


def solution(mesh):
    n_ep, n_tp = mesh.shape["ep"], mesh.shape["tp"]
    in_specs = (
        P("ep", "tp"),
        P("ep", "tp"),
        P("ep", "tp"),
        P("tp", None),
        P(),
        P(),
        P(),
        P(("ep", "tp"), None),
        P(),
        P(("ep", "tp"), None),
        P(("ep", "tp"), None),
        P("ep", None, "tp"),
        P("ep", None, "tp"),
        P("ep", None, "tp"),
    )
    out_specs = (P(("ep", "tp"), None), P(("ep", "tp"), None))
    return jax.shard_map(
        functools.partial(on_device, n_ep, n_tp),
        mesh=mesh,
        in_specs=in_specs,
        out_specs=out_specs,
        check_vma=False,
    )
```

```python
import functools

import jax
import jax.numpy as jnp
from jax import lax
from jax.experimental import pallas as pl
from jax.experimental.pallas import tpu as pltpu
from jax.sharding import PartitionSpec as P

CAP = 16
EPSILON = 1e-06
NEGATIVE = -1e30
MESH = pl.DeviceIdType.MESH
VMEM_LIMIT = 62 * 1024 * 1024


def rms_scale(inputs, gain):
    inputs = inputs.astype(jnp.float32)
    return inputs * lax.rsqrt(jnp.mean(inputs * inputs, axis=-1, keepdims=True) + EPSILON) * gain


def places(n_tp):
    ep, tp = lax.axis_index("ep"), lax.axis_index("tp")
    core = tp + 1 - 2 * lax.rem(tp, 2)
    across = lax.rem(tp + n_tp // 2, n_tp)
    corner = lax.rem(core + n_tp // 2, n_tp)
    return ep, tp, core, across, corner


def paired(place, step, count):
    result, bit = 0, 1
    while bit < count:
        result = result + bit * lax.rem(lax.div(place, bit) + lax.div(step, bit), 2)
        bit *= 2
    return result


def meet(n_ep, n_tp):
    ep, tp = lax.axis_index("ep"), lax.axis_index("tp")
    barrier = pltpu.get_barrier_semaphore()
    for step in range(1, n_ep):
        pl.semaphore_signal(
            barrier, inc=1, device_id=(lax.rem(ep + step, n_ep), tp), device_id_type=MESH
        )
    for step in range(1, n_tp):
        pl.semaphore_signal(
            barrier, inc=1, device_id=(ep, lax.rem(tp + step, n_tp)), device_id_type=MESH
        )
    pl.semaphore_wait(barrier, n_ep + n_tp - 2)


def remote(src, dst, send, recv, ep, tp):
    return pltpu.make_async_remote_copy(
        src_ref=src, dst_ref=dst, send_sem=send, recv_sem=recv, device_id=(ep, tp), device_id_type=MESH
    )


def gather_kernel(
    n_ep,
    n_tp,
    heads,
    outg,
    kv,
    q,
    fq,
    fk,
    pieces,
    att_all,
    kvbuf,
    att,
    high,
    denom,
    accum,
    a_send,
    a_recv,
    x_send,
    x_recv,
    c_send,
    c_recv,
    d_send,
    d_recv,
    u_send,
    k_send,
    k_recv,
    t_send,
    t_recv,
    own_sem,
):
    ep, tp, core, across, corner = places(n_tp)
    rows, head_dim = kv.shape[0], q.shape[1]
    part = rows // n_tp
    scale = head_dim ** (-0.5)
    meet(n_ep, n_tp)

    level, side = lax.div(ep, 2), lax.rem(ep, 2)
    levels = n_ep // 2
    beside = ep + 1 - 2 * side

    def up_copy(src, source):
        above = lax.rem(ep + 2, n_ep)
        return remote(src, kvbuf.at[source], u_send.at[source], k_recv.at[source], above, tp)

    def side_copy(src, source):
        return remote(src, kvbuf.at[source], k_send.at[source], k_recv.at[source], beside, tp)

    def a_copy(step):
        other = paired(ep, step, n_ep)
        return remote(outg.at[other], pieces.at[tp, ep], a_send.at[other], a_recv.at[ep], other, tp)

    def a_wait(step):
        other = paired(ep, step, n_ep)
        remote(
            outg.at[other], pieces.at[tp, other], a_send.at[other], a_recv.at[other], other, tp
        ).wait_recv()

    def x_copy(src, owner, source):
        return remote(src, pieces.at[owner, source], x_send.at[source], x_recv.at[source], ep, across)

    def c_copy(src, owner, source):
        return remote(src, pieces.at[owner, source], c_send.at[source], c_recv.at[source], ep, core)

    def d_copy(src, owner, source):
        return remote(src, pieces.at[owner, source], d_send.at[source], d_recv.at[source], ep, core)

    @pl.when(level + 1 < levels)
    def _():
        up_copy(kv, ep).start()

    @pl.when(side == 0)
    def _():
        side_copy(kv, ep).start()

    own = pltpu.make_async_copy(outg.at[ep], pieces.at[tp, ep], own_sem)
    own.start()
    x_copy(outg.at[ep], tp, ep).start()
    c_copy(outg.at[ep], tp, ep).start()

    def start_a(step, carry):
        a_copy(step).start()
        return carry

    near = min(4, n_ep)
    lax.fori_loop(1, near, start_a, 0)

    tile = rows // 2

    def block(source, keys_ref, diagonal):
        keys = keys_ref[:, :head_dim]
        vals = keys_ref[:, head_dim:]
        for head in range(heads):
            key_gate = fk[source, head : head + 1, :]
            for half in range(2):
                span = pl.ds(head * rows + half * tile, tile)
                scores = lax.dot_general(
                    q[span, :], keys, (((1,), (1,)), ((), ())), preferred_element_type=jnp.float32
                )
                scores = scores * scale + fq[span, :] - key_gate
                if diagonal:
                    qpos = half * tile + lax.broadcasted_iota(jnp.int32, scores.shape, 0)
                    kpos = lax.broadcasted_iota(jnp.int32, scores.shape, 1)
                    scores = jnp.where(kpos <= qpos, scores, NEGATIVE)
                top = jnp.max(scores, axis=1, keepdims=True)
                if diagonal:
                    newest = top
                else:
                    before = high[span, :]
                    newest = jnp.maximum(before, top)
                weights = jnp.exp(scores - newest)
                total = jnp.sum(weights, axis=1, keepdims=True)
                product = jnp.dot(
                    weights.astype(jnp.bfloat16), vals, preferred_element_type=jnp.float32
                )
                if not diagonal:
                    factor = jnp.exp(before - newest)
                    total = denom[span, :] * factor + total
                    product = accum[span, :] * factor + product
                high[span, :] = newest
                denom[span, :] = total
                accum[span, :] = product

    def spread(source):
        side_copy(kvbuf.at[source], source).start()

        @pl.when(level + 1 < levels)
        def _():
            up_copy(kvbuf.at[source], source).start()

    def relay(source):
        x_copy(outg.at[ep], across, source).wait_recv()
        d_copy(pieces.at[across, source], across, source).start()

    @pl.when(level > 0)
    def _():
        side_copy(kv, ep - 2).wait_recv()
        spread(ep - 2)

    lax.fori_loop(near, n_ep, start_a, 0)

    block(ep, kv, True)

    @pl.when(side == 1)
    def _():
        side_copy(kv, ep - 1).wait_recv()
        block(ep - 1, kvbuf.at[ep - 1], False)

    def onward(step, carry):
        source = paired(ep, step, n_ep)
        a_wait(step)
        x_copy(pieces.at[tp, source], tp, source).start()
        c_copy(pieces.at[tp, source], tp, source).start()

        below = level - lax.div(step + 1, 2)
        turned = lax.rem(step + 1, 2)
        lower = 2 * below + lax.rem(side + turned, 2)

        @pl.when(below >= 0)
        def _():
            @pl.when(step > 1)
            def _():
                side_copy(kv, lower).wait_recv()

                @pl.when(turned == 0)
                def _():
                    spread(lower)

            block(lower, kvbuf.at[lower], False)

        relay(paired(ep, step - 1, n_ep))
        return carry

    lax.fori_loop(1, n_ep, onward, 0)

    for head in range(heads):
        span = pl.ds(head * rows, rows)
        result = (accum[span, :] / denom[span, :]).astype(jnp.bfloat16)
        for owner in range(n_tp):
            att[owner, head] = result[owner * part : (owner + 1) * part]
    relay(paired(ep, n_ep - 1, n_ep))

    def t_copy(source, step):
        dest = lax.rem(tp + step, n_tp)
        return remote(att.at[dest], att_all.at[source], t_send.at[step], t_recv.at[source], ep, dest)

    for step in range(1, n_tp):
        t_copy(tp, step).start()
    att_all[tp] = att[tp]

    def finish(source, carry):
        c_copy(outg.at[ep], core, source).wait()
        d_copy(outg.at[ep], corner, source).wait()
        x_copy(outg.at[ep], tp, source).wait_send()
        return carry

    lax.fori_loop(0, n_ep, finish, 0)

    def sent(step, carry):
        a_copy(step).wait_send()
        return carry

    lax.fori_loop(1, n_ep, sent, 0)

    @pl.when(level + 1 < levels)
    def _():
        up_copy(kv, ep).wait_send()

    @pl.when(side == 0)
    def _():
        side_copy(kv, ep).wait_send()

    def spread_sent(k, carry):
        source = ep - 2 * k
        side_copy(kv, source).wait_send()

        @pl.when(level + 1 < levels)
        def _():
            up_copy(kv, source).wait_send()

        return carry

    lax.fori_loop(1, level + 1, spread_sent, 0)
    for step in range(1, n_tp):
        t_copy(lax.rem(tp - step + n_tp, n_tp), step).wait()
    own.wait()


def expert_kernel(x, gate_w, up_w, down_w, out):
    blocks, _, cap, width = x.shape
    chunk = min(blocks, 512 // cap)

    def some(number, carry):
        span = pl.ds(number * chunk, chunk)
        rows = x[span, 0].reshape(chunk * cap, width)
        gate = jnp.dot(rows, gate_w[0], preferred_element_type=jnp.float32)
        upward = jnp.dot(rows, up_w[0], preferred_element_type=jnp.float32)
        hidden = (gate / (1.0 + jnp.exp(-gate)) * upward).astype(jnp.bfloat16)
        result = lax.dot_general(
            hidden, down_w[0], (((1,), (1,)), ((), ())), preferred_element_type=jnp.float32
        )
        out[span, 0] = result.astype(jnp.bfloat16).reshape(chunk, cap, width)
        return carry

    lax.fori_loop(0, blocks // chunk, some, 0)


def return_kernel(
    n_ep,
    n_tp,
    part_ref,
    att_all,
    mixer,
    slots_weights,
    mixed,
    routed,
    near_own,
    near_far,
    sum_x,
    got_x,
    sum_r,
    back,
    n_send,
    n_recv,
    f_send,
    f_recv,
    x_send,
    x_recv,
    r_send,
    r_recv,
):
    ep, tp, core, across, corner = places(n_tp)
    meet(n_ep, n_tp)

    def far_copy(dest):
        return remote(part_ref.at[corner, dest], near_far.at[dest], f_send.at[dest], f_recv.at[dest], ep, core)

    def own_copy(dest):
        return remote(part_ref.at[core, dest], near_own.at[dest], n_send.at[dest], n_recv.at[dest], ep, core)

    def x_copy(dest):
        return remote(sum_x.at[dest], got_x.at[dest], x_send.at[dest], x_recv.at[dest], ep, across)

    def r_copy(source, dest):
        return remote(sum_r.at[dest], back.at[source], r_send.at[dest], r_recv.at[source], dest, tp)

    def order(step):
        return paired(ep, n_ep - step, n_ep)

    def start_far(step, carry):
        far_copy(order(step)).start()
        return carry

    def start_own(step, carry):
        own_copy(order(step)).start()
        return carry

    lax.fori_loop(1, n_ep + 1, start_far, 0)
    lax.fori_loop(1, n_ep + 1, start_own, 0)

    def first(step, carry):
        dest = order(step)
        far_copy(dest).wait_recv()
        sum_x[dest] = (
            part_ref[across, dest].astype(jnp.float32) + near_far[dest].astype(jnp.float32)
        ).astype(jnp.bfloat16)
        x_copy(dest).start()
        return carry

    lax.fori_loop(1, n_ep + 1, first, 0)

    sources, heads, part, head_dim = att_all.shape
    total = None
    for source in range(sources):
        for head in range(heads):
            number = source * heads + head
            term = jnp.dot(
                att_all[source, head],
                mixer[number * head_dim : (number + 1) * head_dim, :],
                preferred_element_type=jnp.float32,
            )
            total = term if total is None else total + term
    mixed[...] = total.astype(jnp.bfloat16)

    def second(dest):
        own_copy(dest).wait_recv()
        x_copy(dest).wait_recv()
        return (
            part_ref[tp, dest].astype(jnp.float32)
            + near_own[dest].astype(jnp.float32)
            + got_x[dest].astype(jnp.float32)
        ).astype(jnp.bfloat16)

    def send_back(step, carry):
        dest = order(step)
        sum_r[dest] = second(dest)
        r_copy(ep, dest).start()
        return carry

    lax.fori_loop(1, n_ep, send_back, 0)
    back[ep] = second(ep)

    def arrived(step, carry):
        other = order(step)
        r_copy(other, other).wait()
        return carry

    lax.fori_loop(1, n_ep, arrived, 0)

    def sent(dest, carry):
        far_copy(dest).wait_send()
        own_copy(dest).wait_send()
        x_copy(dest).wait_send()
        return carry

    lax.fori_loop(0, n_ep, sent, 0)

    _, per, width = back.shape
    rows = back[...].reshape(n_ep * per, width)
    summed = None
    top = slots_weights.shape[1] // 2
    for choice in range(top):
        lanes = lax.broadcasted_iota(jnp.int32, (mixed.shape[0], n_ep * per), 1)
        pick = jnp.where(lanes.astype(jnp.float32) == slots_weights[:, choice : choice + 1], 1.0, 0.0).astype(jnp.bfloat16)
        found = jnp.dot(pick, rows, preferred_element_type=jnp.float32)
        term = found * slots_weights[:, top + choice : top + choice + 1]
        summed = term if summed is None else summed + term
    routed[...] = summed.astype(jnp.bfloat16)


def on_device(
    n_ep,
    n_tp,
    queries,
    keys,
    values,
    forget_cache,
    query_gain,
    key_gain,
    mixer_out,
    expert_input,
    norm_gain,
    routes,
    route_weights,
    w_gate,
    w_up,
    w_down,
):
    rows, head_dim = keys.shape
    heads = forget_cache.shape[0]
    ep = lax.axis_index("ep")
    local, width, ff = w_gate.shape
    experts = local * n_ep
    tokens = expert_input.shape[0]
    per = local * CAP
    part = rows // n_tp
    vmem = pl.BlockSpec(memory_space=pltpu.VMEM)
    anywhere = pl.BlockSpec(memory_space=pl.ANY)
    dma = pltpu.SemaphoreType.DMA

    normed_q = rms_scale(queries.reshape(rows, heads, head_dim), query_gain).astype(jnp.bfloat16)
    q = normed_q.transpose(1, 0, 2).reshape(heads * rows, head_dim)
    kv = jnp.concatenate([rms_scale(keys, key_gain).astype(jnp.bfloat16), values], axis=1)
    fq = lax.dynamic_slice_in_dim(forget_cache, ep * rows, rows, 1).reshape(heads * rows, 1)
    fk = forget_cache.reshape(heads, n_ep, rows).transpose(1, 0, 2)

    normed = rms_scale(expert_input, norm_gain).astype(jnp.bfloat16)
    names = jnp.arange(experts, dtype=jnp.int32)
    named = [(routes[:, k : k + 1] == names[None, :]) for k in range(routes.shape[1])]
    anyone = functools.reduce(jnp.logical_or, named).astype(jnp.bfloat16)
    at = jnp.arange(tokens, dtype=jnp.int32)
    earlier = (at[None, :] < at[:, None]).astype(jnp.bfloat16)
    prior = jnp.dot(earlier, anyone, preferred_element_type=jnp.float32)
    ranks = [jnp.sum(jnp.where(mine, prior, 0.0), axis=1).astype(jnp.int32) for mine in named]
    slots = jnp.stack([routes[:, k] * CAP + rank for k, rank in enumerate(ranks)], axis=1)
    slots_weights = jnp.concatenate([slots.astype(jnp.float32), route_weights], axis=1)
    line = jnp.arange(experts * CAP, dtype=jnp.int32)[:, None]
    place = functools.reduce(
        jnp.logical_or, [line == slots[:, k][None, :] for k in range(slots.shape[1])]
    ).astype(jnp.bfloat16)
    outg = jnp.dot(place, normed, preferred_element_type=jnp.float32).astype(jnp.bfloat16)
    outg = outg.reshape(n_ep, per, width)

    pieces, att_all = pl.pallas_call(
        functools.partial(gather_kernel, n_ep, n_tp, heads),
        out_shape=(
            jax.ShapeDtypeStruct((n_tp, n_ep, per, width), jnp.bfloat16),
            jax.ShapeDtypeStruct((n_tp, heads, part, head_dim), jnp.bfloat16),
        ),
        in_specs=[vmem] * 5,
        out_specs=(anywhere, vmem),
        scratch_shapes=[
            pltpu.VMEM((n_ep, rows, 2 * head_dim), jnp.bfloat16),
            pltpu.VMEM((n_tp, heads, part, head_dim), jnp.bfloat16),
            pltpu.VMEM((heads * rows, 1), jnp.float32),
            pltpu.VMEM((heads * rows, 1), jnp.float32),
            pltpu.VMEM((heads * rows, head_dim), jnp.float32),
        ]
        + [dma((n_ep,))] * 11
        + [dma((n_tp,))] * 2
        + [dma],
        compiler_params=pltpu.CompilerParams(
            collective_id=0, has_side_effects=True, vmem_limit_bytes=VMEM_LIMIT
        ),
        name="gather",
    )(outg, kv, q, fq, fk)

    blocks = n_tp * n_ep
    row_spec = pl.BlockSpec((blocks, 1, CAP, width), lambda e: (0, e, 0, 0))
    weight_spec = pl.BlockSpec((1, width, ff), lambda e: (e, 0, 0))
    partial_sums = pl.pallas_call(
        expert_kernel,
        out_shape=jax.ShapeDtypeStruct((blocks, local, CAP, width), jnp.bfloat16),
        grid=(local,),
        in_specs=[row_spec, weight_spec, weight_spec, weight_spec],
        out_specs=row_spec,
        compiler_params=pltpu.CompilerParams(vmem_limit_bytes=VMEM_LIMIT),
        name="experts",
    )(pieces.reshape(blocks, local, CAP, width), w_gate, w_up, w_down)
    partial_sums = partial_sums.reshape(n_tp, n_ep, per, width)

    buffer = pltpu.VMEM((n_ep, per, width), jnp.bfloat16)
    return pl.pallas_call(
        functools.partial(return_kernel, n_ep, n_tp),
        out_shape=(
            jax.ShapeDtypeStruct((part, width), jnp.bfloat16),
            jax.ShapeDtypeStruct((tokens, width), jnp.bfloat16),
        ),
        in_specs=[vmem] * 4,
        out_specs=(vmem, vmem),
        scratch_shapes=[buffer] * 6 + [dma((n_ep,))] * 8,
        compiler_params=pltpu.CompilerParams(
            collective_id=1, has_side_effects=True, vmem_limit_bytes=VMEM_LIMIT
        ),
        name="give_back",
    )(partial_sums, att_all, mixer_out, slots_weights)


def solution(mesh):
    n_ep, n_tp = mesh.shape["ep"], mesh.shape["tp"]
    in_specs = (
        P("ep", "tp"),
        P("ep", "tp"),
        P("ep", "tp"),
        P("tp", None),
        P(),
        P(),
        P(),
        P(("ep", "tp"), None),
        P(),
        P(("ep", "tp"), None),
        P(("ep", "tp"), None),
        P("ep", None, "tp"),
        P("ep", None, "tp"),
        P("ep", None, "tp"),
    )
    out_specs = (P(("ep", "tp"), None), P(("ep", "tp"), None))
    return jax.shard_map(
        functools.partial(on_device, n_ep, n_tp),
        mesh=mesh,
        in_specs=in_specs,
        out_specs=out_specs,
        check_vma=False,
    )
```

```python
import functools

import jax
import jax.numpy as jnp
from jax import lax
from jax.experimental import pallas as pl
from jax.experimental.pallas import tpu as pltpu
from jax.sharding import PartitionSpec as P

CAP = 16
EPSILON = 1e-06
NEGATIVE = -1e30
MESH = pl.DeviceIdType.MESH
VMEM_LIMIT = 62 * 1024 * 1024


def rms_scale(inputs, gain):
    inputs = inputs.astype(jnp.float32)
    return inputs * lax.rsqrt(jnp.mean(inputs * inputs, axis=-1, keepdims=True) + EPSILON) * gain


def places(n_tp):
    ep, tp = lax.axis_index("ep"), lax.axis_index("tp")
    core = tp + 1 - 2 * lax.rem(tp, 2)
    across = lax.rem(tp + n_tp // 2, n_tp)
    corner = lax.rem(core + n_tp // 2, n_tp)
    return ep, tp, core, across, corner


def weights_of(count):
    digits = count.bit_length() - 1
    assert count == 1 << digits
    return [1] + [1 << (digits - number) for number in range(1, digits)]


def paired(place, slot, count):
    result = 0
    for number, weight in enumerate(weights_of(count)):
        result = result + weight * lax.rem(lax.div(place, weight) + lax.div(slot, 1 << number), 2)
    return result


def meet(n_ep, n_tp):
    ep, tp = lax.axis_index("ep"), lax.axis_index("tp")
    barrier = pltpu.get_barrier_semaphore()
    for step in range(1, n_ep):
        pl.semaphore_signal(
            barrier, inc=1, device_id=(lax.rem(ep + step, n_ep), tp), device_id_type=MESH
        )
    for step in range(1, n_tp):
        pl.semaphore_signal(
            barrier, inc=1, device_id=(ep, lax.rem(tp + step, n_tp)), device_id_type=MESH
        )
    pl.semaphore_wait(barrier, n_ep + n_tp - 2)


def remote(src, dst, send, recv, ep, tp):
    return pltpu.make_async_remote_copy(
        src_ref=src, dst_ref=dst, send_sem=send, recv_sem=recv, device_id=(ep, tp), device_id_type=MESH
    )


def layer_kernel(
    n_ep,
    n_tp,
    heads,
    outg,
    kv,
    q,
    fq,
    fk,
    slots_weights,
    gate_hbm,
    up_hbm,
    down_hbm,
    mixer_hbm,
    mixed,
    routed,
    gate_w,
    up_w,
    down_w,
    mixer,
    kvbuf,
    att,
    att_all,
    high,
    denom,
    accum,
    pieces,
    sums,
    near_own,
    near_far,
    sum_x,
    got_x,
    sum_r,
    back,
    a_send,
    a_recv,
    x_send,
    x_recv,
    c_send,
    c_recv,
    d_send,
    d_recv,
    u_send,
    k_send,
    k_recv,
    f_send,
    f_recv,
    n_send,
    n_recv,
    y_send,
    y_recv,
    r_send,
    r_recv,
    t_send,
    t_recv,
    w_sem,
    own_sem,
):
    ep, tp, core, across, corner = places(n_tp)
    rows, head_dim = kv.shape[0], q.shape[1]
    part = rows // n_tp
    scale = head_dim ** (-0.5)
    local, width, ff = gate_w.shape
    half = n_ep // 2
    level, side = lax.div(ep, 2), lax.rem(ep, 2)
    levels = n_ep // 2
    beside = ep + 1 - 2 * side
    assert local <= half
    loads = [
        pltpu.make_async_copy(src, dst, w_sem.at[number])
        for number, (src, dst) in enumerate(
            [(gate_hbm, gate_w), (up_hbm, up_w), (down_hbm, down_w), (mixer_hbm, mixer)]
        )
    ]
    meet(n_ep, n_tp)

    def up_copy(src, source):
        above = lax.rem(ep + 2, n_ep)
        return remote(src, kvbuf.at[source], u_send.at[source], k_recv.at[source], above, tp)

    def side_copy(src, source):
        return remote(src, kvbuf.at[source], k_send.at[source], k_recv.at[source], beside, tp)

    def a_copy(slot):
        other = paired(ep, slot, n_ep)
        return remote(outg.at[slot], pieces.at[tp, slot], a_send.at[slot], a_recv.at[slot], other, tp)

    def x_copy(src, owner, slot):
        return remote(src, pieces.at[owner, slot], x_send.at[slot], x_recv.at[slot], ep, across)

    def c_copy(src, owner, slot):
        return remote(src, pieces.at[owner, slot], c_send.at[slot], c_recv.at[slot], ep, core)

    def d_copy(src, owner, slot):
        return remote(src, pieces.at[owner, slot], d_send.at[slot], d_recv.at[slot], ep, core)

    def far_copy(slot):
        return remote(sums.at[corner, slot], near_far.at[slot], f_send.at[slot], f_recv.at[slot], ep, core)

    def own_copy(slot):
        return remote(sums.at[core, slot], near_own.at[slot], n_send.at[slot], n_recv.at[slot], ep, core)

    def y_copy(slot):
        return remote(sum_x.at[slot], got_x.at[slot], y_send.at[slot], y_recv.at[slot], ep, across)

    def r_copy(slot):
        other = paired(ep, slot, n_ep)
        return remote(sum_r.at[slot], back.at[slot], r_send.at[slot], r_recv.at[slot], other, tp)

    def each(first, last, act):
        def body(number, carry):
            act(number)
            return carry

        lax.fori_loop(first, last, body, 0)

    @pl.when(level + 1 < levels)
    def _():
        up_copy(kv, ep).start()

    @pl.when(side == 0)
    def _():
        side_copy(kv, ep).start()

    own = pltpu.make_async_copy(outg.at[0], pieces.at[tp, 0], own_sem)
    own.start()
    x_copy(outg.at[0], tp, 0).start()
    c_copy(outg.at[0], tp, 0).start()
    a_copy(1).start()
    for load in loads:
        load.start()
    tile = rows // 2

    def block(source, keys_ref, diagonal):
        keys = keys_ref[:, :head_dim]
        vals = keys_ref[:, head_dim:]
        for head in range(heads):
            key_gate = fk[source, head : head + 1, :]
            for piece in range(2):
                span = pl.ds(head * rows + piece * tile, tile)
                scores = lax.dot_general(
                    q[span, :], keys, (((1,), (1,)), ((), ())), preferred_element_type=jnp.float32
                )
                scores = scores * scale + fq[span, :] - key_gate
                if diagonal:
                    qpos = piece * tile + lax.broadcasted_iota(jnp.int32, scores.shape, 0)
                    kpos = lax.broadcasted_iota(jnp.int32, scores.shape, 1)
                    scores = jnp.where(kpos <= qpos, scores, NEGATIVE)
                top = jnp.max(scores, axis=1, keepdims=True)
                if diagonal:
                    newest = top
                else:
                    before = high[span, :]
                    newest = jnp.maximum(before, top)
                weights = jnp.exp(scores - newest)
                total = jnp.sum(weights, axis=1, keepdims=True)
                product = jnp.dot(
                    weights.astype(jnp.bfloat16), vals, preferred_element_type=jnp.float32
                )
                if not diagonal:
                    factor = jnp.exp(before - newest)
                    total = denom[span, :] * factor + total
                    product = accum[span, :] * factor + product
                high[span, :] = newest
                denom[span, :] = total
                accum[span, :] = product

    def spread(source):
        side_copy(kvbuf.at[source], source).start()

        @pl.when(level + 1 < levels)
        def _():
            up_copy(kvbuf.at[source], source).start()

    def relay(slot):
        x_copy(outg.at[0], across, slot).wait_recv()
        d_copy(pieces.at[across, slot], across, slot).start()

    @pl.when(level > 0)
    def _():
        side_copy(kv, ep - 2).wait_recv()
        spread(ep - 2)

    each(2, n_ep, lambda slot: a_copy(slot).start())
    block(ep, kv, True)

    @pl.when(side == 1)
    def _():
        side_copy(kv, ep - 1).wait_recv()
        block(ep - 1, kvbuf.at[ep - 1], False)

    def landed(slot):
        c_copy(outg.at[0], core, slot).wait_recv()
        d_copy(outg.at[0], corner, slot).wait_recv()

    def expert(number, begin):
        own_rows = pl.ds(pl.multiple_of(number * CAP, CAP), CAP)
        taken = pieces[:, begin : begin + half, own_rows, :].reshape(n_tp * half * CAP, width)
        gate = jnp.dot(taken, gate_w[number], preferred_element_type=jnp.float32)
        upward = jnp.dot(taken, up_w[number], preferred_element_type=jnp.float32)
        hidden = (gate / (1.0 + jnp.exp(-gate)) * upward).astype(jnp.bfloat16)
        columns = min(width, 512)
        for begin_column in range(0, width, columns):
            lanes = slice(begin_column, begin_column + columns)
            result = lax.dot_general(
                hidden,
                down_w[number, lanes, :],
                (((1,), (1,)), ((), ())),
                preferred_element_type=jnp.float32,
            )
            sums[:, begin : begin + half, own_rows, lanes] = result.astype(jnp.bfloat16).reshape(
                n_tp, half, CAP, columns
            )

    def onward(slot):
        a_copy(slot).wait_recv()
        x_copy(pieces.at[tp, slot], tp, slot).start()
        c_copy(pieces.at[tp, slot], tp, slot).start()

        below = level - lax.div(slot + 1, 2)
        turned = lax.rem(slot + 1, 2)
        lower = 2 * below + lax.rem(side + turned, 2)

        @pl.when(below >= 0)
        def _():
            @pl.when(slot > 1)
            def _():
                side_copy(kv, lower).wait_recv()

                @pl.when(turned == 0)
                def _():
                    spread(lower)

            block(lower, kvbuf.at[lower], False)

        relay(slot - 1)

    each(1, half, onward)

    def onward_and_expert(slot):
        onward(slot)

        @pl.when(slot == half)
        def _():
            own.wait()
            for load in loads:
                load.wait()
            each(0, half, landed)

        @pl.when(slot - half < local)
        def _():
            expert(slot - half, 0)

    each(half, n_ep, onward_and_expert)
    relay(n_ep - 1)

    def hand_over(begin):
        each(0, half, lambda step: far_copy(begin + half - 1 - step).start())
        each(0, half, lambda step: own_copy(begin + half - 1 - step).start())

        def add(step):
            slot = begin + half - 1 - step
            far_copy(slot).wait_recv()
            sum_x[slot] = (
                sums[across, slot].astype(jnp.float32) + near_far[slot].astype(jnp.float32)
            ).astype(jnp.bfloat16)
            y_copy(slot).start()

        each(0, half, add)

    def total_of(slot):
        own_copy(slot).wait_recv()
        y_copy(slot).wait_recv()
        return (
            sums[tp, slot].astype(jnp.float32)
            + near_own[slot].astype(jnp.float32)
            + got_x[slot].astype(jnp.float32)
        ).astype(jnp.bfloat16)

    def send_back(slot):
        sum_r[slot] = total_of(slot)
        r_copy(slot).start()

    hand_over(0)
    for head in range(heads):
        span = pl.ds(head * rows, rows)
        result = (accum[span, :] / denom[span, :]).astype(jnp.bfloat16)
        for owner in range(n_tp):
            att[owner, head] = result[owner * part : (owner + 1) * part]

    def t_copy(source, step):
        dest = lax.rem(tp + step, n_tp)
        return remote(att.at[dest], att_all.at[source], t_send.at[step], t_recv.at[source], ep, dest)

    for step in range(1, n_tp):
        t_copy(tp, step).start()
    att_all[tp] = att[tp]

    each(half, n_ep, landed)
    each(0, local, lambda number: expert(number, half))
    hand_over(half)

    each(1, half, lambda step: send_back(half - step))
    back[0] = total_of(0)

    for step in range(1, n_tp):
        t_copy(lax.rem(tp - step + n_tp, n_tp), step).wait()
    total = None
    for source in range(n_tp):
        for head in range(heads):
            number = source * heads + head
            term = jnp.dot(
                att_all[source, head],
                mixer[number * head_dim : (number + 1) * head_dim, :],
                preferred_element_type=jnp.float32,
            )
            total = term if total is None else total + term
    mixed[...] = total.astype(jnp.bfloat16)

    each(0, half, lambda step: send_back(n_ep - 1 - step))

    def sent(slot):
        x_copy(outg.at[0], tp, slot).wait_send()
        c_copy(outg.at[0], tp, slot).wait_send()
        d_copy(outg.at[0], tp, slot).wait_send()
        far_copy(slot).wait_send()
        own_copy(slot).wait_send()
        y_copy(slot).wait_send()

    each(0, n_ep, sent)
    each(1, n_ep, lambda slot: a_copy(slot).wait_send())

    @pl.when(level + 1 < levels)
    def _():
        up_copy(kv, ep).wait_send()

    @pl.when(side == 0)
    def _():
        side_copy(kv, ep).wait_send()

    def spread_sent(k):
        source = ep - 2 * k
        side_copy(kv, source).wait_send()

        @pl.when(level + 1 < levels)
        def _():
            up_copy(kv, source).wait_send()

    each(1, level + 1, spread_sent)
    each(1, n_ep, lambda slot: r_copy(slot).wait())

    _, per, _ = back.shape
    found_rows = back[...].reshape(n_ep * per, width)
    summed = None
    top = slots_weights.shape[1] // 2
    for choice in range(top):
        lanes = lax.broadcasted_iota(jnp.int32, (mixed.shape[0], n_ep * per), 1)
        pick = jnp.where(
            lanes.astype(jnp.float32) == slots_weights[:, choice : choice + 1], 1.0, 0.0
        ).astype(jnp.bfloat16)
        found = jnp.dot(pick, found_rows, preferred_element_type=jnp.float32)
        term = found * slots_weights[:, top + choice : top + choice + 1]
        summed = term if summed is None else summed + term
    routed[...] = summed.astype(jnp.bfloat16)


def on_device(
    n_ep,
    n_tp,
    queries,
    keys,
    values,
    forget_cache,
    query_gain,
    key_gain,
    mixer_out,
    expert_input,
    norm_gain,
    routes,
    route_weights,
    w_gate,
    w_up,
    w_down,
):
    rows, head_dim = keys.shape
    heads = forget_cache.shape[0]
    ep = lax.axis_index("ep")
    local, width, ff = w_gate.shape
    experts = local * n_ep
    tokens = expert_input.shape[0]
    per = local * CAP
    part = rows // n_tp
    vmem = pl.BlockSpec(memory_space=pltpu.VMEM)
    anywhere = pl.BlockSpec(memory_space=pl.ANY)
    dma = pltpu.SemaphoreType.DMA

    normed_q = rms_scale(queries.reshape(rows, heads, head_dim), query_gain).astype(jnp.bfloat16)
    q = normed_q.transpose(1, 0, 2).reshape(heads * rows, head_dim)
    kv = jnp.concatenate([rms_scale(keys, key_gain).astype(jnp.bfloat16), values], axis=1)
    fq = lax.dynamic_slice_in_dim(forget_cache, ep * rows, rows, 1).reshape(heads * rows, 1)
    fk = forget_cache.reshape(heads, n_ep, rows).transpose(1, 0, 2)

    normed = rms_scale(expert_input, norm_gain).astype(jnp.bfloat16)
    names = jnp.arange(experts, dtype=jnp.int32)
    named = [(routes[:, k : k + 1] == names[None, :]) for k in range(routes.shape[1])]
    anyone = functools.reduce(jnp.logical_or, named).astype(jnp.bfloat16)
    at = jnp.arange(tokens, dtype=jnp.int32)
    earlier = (at[None, :] < at[:, None]).astype(jnp.bfloat16)
    prior = jnp.dot(earlier, anyone, preferred_element_type=jnp.float32)
    ranks = [jnp.sum(jnp.where(mine, prior, 0.0), axis=1).astype(jnp.int32) for mine in named]
    differ = (routes // local) ^ ep
    slot = jnp.zeros_like(routes)
    for number, weight in enumerate(weights_of(n_ep)):
        slot = slot + (1 << number) * (differ // weight % 2)
    base = slot * per + routes % local * CAP
    slots = jnp.stack([base[:, k] + rank for k, rank in enumerate(ranks)], axis=1)
    slots_weights = jnp.concatenate([slots.astype(jnp.float32), route_weights], axis=1)
    line = jnp.arange(experts * CAP, dtype=jnp.int32)[:, None]
    place = functools.reduce(
        jnp.logical_or, [line == slots[:, k][None, :] for k in range(slots.shape[1])]
    ).astype(jnp.bfloat16)
    outg = jnp.dot(place, normed, preferred_element_type=jnp.float32).astype(jnp.bfloat16)
    outg = outg.reshape(n_ep, per, width)

    buffer = pltpu.VMEM((n_ep, per, width), jnp.bfloat16)
    return pl.pallas_call(
        functools.partial(layer_kernel, n_ep, n_tp, heads),
        out_shape=(
            jax.ShapeDtypeStruct((part, width), jnp.bfloat16),
            jax.ShapeDtypeStruct((tokens, width), jnp.bfloat16),
        ),
        in_specs=[vmem] * 6 + [anywhere] * 4,
        out_specs=(vmem, vmem),
        scratch_shapes=[pltpu.VMEM(w_gate.shape, jnp.bfloat16)] * 3
        + [
            pltpu.VMEM(mixer_out.shape, jnp.bfloat16),
            pltpu.VMEM((n_ep, rows, 2 * head_dim), jnp.bfloat16),
            pltpu.VMEM((n_tp, heads, part, head_dim), jnp.bfloat16),
            pltpu.VMEM((n_tp, heads, part, head_dim), jnp.bfloat16),
            pltpu.VMEM((heads * rows, 1), jnp.float32),
            pltpu.VMEM((heads * rows, 1), jnp.float32),
            pltpu.VMEM((heads * rows, head_dim), jnp.float32),
            pltpu.VMEM((n_tp, n_ep, per, width), jnp.bfloat16),
            pltpu.VMEM((n_tp, n_ep, per, width), jnp.bfloat16),
        ]
        + [buffer] * 6
        + [dma((n_ep,))] * 19
        + [dma((n_tp,))] * 3
        + [dma],
        compiler_params=pltpu.CompilerParams(
            collective_id=0, has_side_effects=True, vmem_limit_bytes=VMEM_LIMIT
        ),
        name="layer",
    )(outg, kv, q, fq, fk, slots_weights, w_gate, w_up, w_down, mixer_out)


def solution(mesh):
    n_ep, n_tp = mesh.shape["ep"], mesh.shape["tp"]
    in_specs = (
        P("ep", "tp"),
        P("ep", "tp"),
        P("ep", "tp"),
        P("tp", None),
        P(),
        P(),
        P(),
        P(("ep", "tp"), None),
        P(),
        P(("ep", "tp"), None),
        P(("ep", "tp"), None),
        P("ep", None, "tp"),
        P("ep", None, "tp"),
        P("ep", None, "tp"),
    )
    out_specs = (P(("ep", "tp"), None), P(("ep", "tp"), None))
    return jax.shard_map(
        functools.partial(on_device, n_ep, n_tp),
        mesh=mesh,
        in_specs=in_specs,
        out_specs=out_specs,
        check_vma=False,
    )
```

```python
import functools

import jax
import jax.numpy as jnp
from jax import lax
from jax.experimental import pallas as pl
from jax.experimental.pallas import tpu as pltpu
from jax.sharding import PartitionSpec as P

CAP = 16
EPSILON = 1e-06
NEGATIVE = -1e30
MESH = pl.DeviceIdType.MESH
VMEM_LIMIT = 62 * 1024 * 1024


def rms_scale(inputs, gain):
    inputs = inputs.astype(jnp.float32)
    return inputs * lax.rsqrt(jnp.mean(inputs * inputs, axis=-1, keepdims=True) + EPSILON) * gain


def places(n_tp):
    ep, tp = lax.axis_index("ep"), lax.axis_index("tp")
    core = tp + 1 - 2 * lax.rem(tp, 2)
    across = lax.rem(tp + n_tp // 2, n_tp)
    corner = lax.rem(core + n_tp // 2, n_tp)
    return ep, tp, core, across, corner


def weights_of(count):
    digits = count.bit_length() - 1
    assert count == 1 << digits
    return [1] + [1 << (digits - number) for number in range(1, digits)]


def paired(place, slot, count):
    result = 0
    for number, weight in enumerate(weights_of(count)):
        result = result + weight * lax.rem(lax.div(place, weight) + lax.div(slot, 1 << number), 2)
    return result


def meet(n_ep, n_tp):
    ep, tp = lax.axis_index("ep"), lax.axis_index("tp")
    barrier = pltpu.get_barrier_semaphore()
    for step in range(1, n_ep):
        pl.semaphore_signal(
            barrier, inc=1, device_id=(lax.rem(ep + step, n_ep), tp), device_id_type=MESH
        )
    for step in range(1, n_tp):
        pl.semaphore_signal(
            barrier, inc=1, device_id=(ep, lax.rem(tp + step, n_tp)), device_id_type=MESH
        )
    pl.semaphore_wait(barrier, n_ep + n_tp - 2)


def remote(src, dst, send, recv, ep, tp):
    return pltpu.make_async_remote_copy(
        src_ref=src, dst_ref=dst, send_sem=send, recv_sem=recv, device_id=(ep, tp), device_id_type=MESH
    )


def layer_kernel(
    n_ep,
    n_tp,
    heads,
    outg,
    kv,
    q,
    fq,
    fk,
    slots_weights,
    gate_hbm,
    up_hbm,
    down_hbm,
    mixer_hbm,
    mixed,
    routed,
    gate_w,
    up_w,
    down_w,
    mixer,
    kvbuf,
    att,
    att_all,
    high,
    denom,
    accum,
    pieces,
    sums,
    near_own,
    near_far,
    sum_x,
    got_x,
    sum_r,
    back,
    a_send,
    a_recv,
    x_send,
    x_recv,
    c_send,
    c_recv,
    d_send,
    d_recv,
    u_send,
    k_send,
    k_recv,
    f_send,
    f_recv,
    n_send,
    n_recv,
    y_send,
    y_recv,
    r_send,
    r_recv,
    t_send,
    t_recv,
    w_sem,
    own_sem,
):
    ep, tp, core, across, corner = places(n_tp)
    rows, head_dim = kv.shape[0], q.shape[1]
    part = rows // n_tp
    scale = head_dim ** (-0.5)
    local, width, ff = gate_w.shape
    half = n_ep // 2
    level, side = lax.div(ep, 2), lax.rem(ep, 2)
    levels = n_ep // 2
    beside = ep + 1 - 2 * side
    assert local <= half
    loads = [
        pltpu.make_async_copy(src, dst, w_sem.at[number])
        for number, (src, dst) in enumerate(
            [(gate_hbm, gate_w), (up_hbm, up_w), (down_hbm, down_w), (mixer_hbm, mixer)]
        )
    ]
    meet(n_ep, n_tp)

    def up_copy(src, source):
        above = lax.rem(ep + 2, n_ep)
        return remote(src, kvbuf.at[source], u_send.at[source], k_recv.at[source], above, tp)

    def side_copy(src, source):
        return remote(src, kvbuf.at[source], k_send.at[source], k_recv.at[source], beside, tp)

    def a_copy(slot):
        other = paired(ep, slot, n_ep)
        return remote(outg.at[slot], pieces.at[tp, slot], a_send.at[slot], a_recv.at[slot], other, tp)

    def x_copy(src, owner, slot):
        return remote(src, pieces.at[owner, slot], x_send.at[slot], x_recv.at[slot], ep, across)

    def c_copy(src, owner, slot):
        return remote(src, pieces.at[owner, slot], c_send.at[slot], c_recv.at[slot], ep, core)

    def d_copy(src, owner, slot):
        return remote(src, pieces.at[owner, slot], d_send.at[slot], d_recv.at[slot], ep, core)

    def far_copy(slot):
        return remote(sums.at[corner, slot], near_far.at[slot], f_send.at[slot], f_recv.at[slot], ep, core)

    def own_copy(slot):
        return remote(sums.at[core, slot], near_own.at[slot], n_send.at[slot], n_recv.at[slot], ep, core)

    def y_copy(slot):
        return remote(sum_x.at[slot], got_x.at[slot], y_send.at[slot], y_recv.at[slot], ep, across)

    def r_copy(slot):
        other = paired(ep, slot, n_ep)
        return remote(sum_r.at[slot], back.at[slot], r_send.at[slot], r_recv.at[slot], other, tp)

    def each(first, last, act):
        def body(number, carry):
            act(number)
            return carry

        lax.fori_loop(first, last, body, 0)

    @pl.when(level + 1 < levels)
    def _():
        up_copy(kv, ep).start()

    @pl.when(side == 0)
    def _():
        side_copy(kv, ep).start()

    own = pltpu.make_async_copy(outg.at[0], pieces.at[tp, 0], own_sem)
    own.start()
    x_copy(outg.at[0], tp, 0).start()
    c_copy(outg.at[0], tp, 0).start()
    a_copy(1).start()
    for load in loads:
        load.start()
    tile = rows // 2

    def block(source, keys_ref, diagonal):
        keys = keys_ref[:, :head_dim]
        vals = keys_ref[:, head_dim:]
        for head in range(heads):
            key_gate = fk[source, head : head + 1, :]
            for piece in range(2):
                span = pl.ds(head * rows + piece * tile, tile)
                scores = lax.dot_general(
                    q[span, :], keys, (((1,), (1,)), ((), ())), preferred_element_type=jnp.float32
                )
                scores = scores * scale + fq[span, :] - key_gate
                if diagonal:
                    qpos = piece * tile + lax.broadcasted_iota(jnp.int32, scores.shape, 0)
                    kpos = lax.broadcasted_iota(jnp.int32, scores.shape, 1)
                    scores = jnp.where(kpos <= qpos, scores, NEGATIVE)
                top = jnp.max(scores, axis=1, keepdims=True)
                if diagonal:
                    newest = top
                else:
                    before = high[span, :]
                    newest = jnp.maximum(before, top)
                weights = jnp.exp(scores - newest)
                total = jnp.sum(weights, axis=1, keepdims=True)
                product = jnp.dot(
                    weights.astype(jnp.bfloat16), vals, preferred_element_type=jnp.float32
                )
                if not diagonal:
                    factor = jnp.exp(before - newest)
                    total = denom[span, :] * factor + total
                    product = accum[span, :] * factor + product
                high[span, :] = newest
                denom[span, :] = total
                accum[span, :] = product

    def spread(source):
        side_copy(kvbuf.at[source], source).start()

        @pl.when(level + 1 < levels)
        def _():
            up_copy(kvbuf.at[source], source).start()

    def relay(slot):
        x_copy(outg.at[0], across, slot).wait_recv()
        d_copy(pieces.at[across, slot], across, slot).start()

    @pl.when(level > 0)
    def _():
        side_copy(kv, ep - 2).wait_recv()
        spread(ep - 2)

    each(2, n_ep, lambda slot: a_copy(slot).start())
    block(ep, kv, True)

    @pl.when(side == 1)
    def _():
        side_copy(kv, ep - 1).wait_recv()
        block(ep - 1, kvbuf.at[ep - 1], False)

    def landed(slot):
        c_copy(outg.at[0], core, slot).wait_recv()
        d_copy(outg.at[0], corner, slot).wait_recv()

    def expert(number, begin):
        own_rows = pl.ds(pl.multiple_of(number * CAP, CAP), CAP)
        taken = pieces[:, begin : begin + half, own_rows, :].reshape(n_tp * half * CAP, width)
        gate = jnp.dot(taken, gate_w[number], preferred_element_type=jnp.float32)
        upward = jnp.dot(taken, up_w[number], preferred_element_type=jnp.float32)
        hidden = (gate / (1.0 + jnp.exp(-gate)) * upward).astype(jnp.bfloat16)
        columns = min(width, 512)
        for begin_column in range(0, width, columns):
            lanes = slice(begin_column, begin_column + columns)
            result = lax.dot_general(
                hidden,
                down_w[number, lanes, :],
                (((1,), (1,)), ((), ())),
                preferred_element_type=jnp.float32,
            )
            sums[:, begin : begin + half, own_rows, lanes] = result.astype(jnp.bfloat16).reshape(
                n_tp, half, CAP, columns
            )

    def onward(slot):
        a_copy(slot).wait_recv()
        x_copy(pieces.at[tp, slot], tp, slot).start()
        c_copy(pieces.at[tp, slot], tp, slot).start()

        below = level - lax.div(slot + 1, 2)
        turned = lax.rem(slot + 1, 2)
        lower = 2 * below + lax.rem(side + turned, 2)

        @pl.when(below >= 0)
        def _():
            @pl.when(slot > 1)
            def _():
                side_copy(kv, lower).wait_recv()

                @pl.when(turned == 0)
                def _():
                    spread(lower)

            block(lower, kvbuf.at[lower], False)

        relay(slot - 1)

    each(1, half, onward)

    def hand_over(begin):
        each(0, half, lambda step: far_copy(begin + half - 1 - step).start())
        each(0, half, lambda step: own_copy(begin + half - 1 - step).start())

        def add(step):
            slot = begin + half - 1 - step
            far_copy(slot).wait_recv()
            sum_x[slot] = (
                sums[across, slot].astype(jnp.float32) + near_far[slot].astype(jnp.float32)
            ).astype(jnp.bfloat16)
            y_copy(slot).start()

        each(0, half, add)

    def total_of(slot):
        own_copy(slot).wait_recv()
        y_copy(slot).wait_recv()
        return (
            sums[tp, slot].astype(jnp.float32)
            + near_own[slot].astype(jnp.float32)
            + got_x[slot].astype(jnp.float32)
        ).astype(jnp.bfloat16)

    def send_back(slot):
        sum_r[slot] = total_of(slot)
        r_copy(slot).start()

    def onward_and_expert(slot):
        onward(slot)

        @pl.when(slot == half)
        def _():
            own.wait()
            for load in loads:
                load.wait()
            each(0, half, landed)
            each(0, local, lambda number: expert(number, 0))
            hand_over(0)

    each(half, n_ep, onward_and_expert)
    relay(n_ep - 1)

    each(1, half, lambda step: send_back(half - step))
    back[0] = total_of(0)
    for head in range(heads):
        span = pl.ds(head * rows, rows)
        result = (accum[span, :] / denom[span, :]).astype(jnp.bfloat16)
        for owner in range(n_tp):
            att[owner, head] = result[owner * part : (owner + 1) * part]

    def t_copy(source, step):
        dest = lax.rem(tp + step, n_tp)
        return remote(att.at[dest], att_all.at[source], t_send.at[step], t_recv.at[source], ep, dest)

    for step in range(1, n_tp):
        t_copy(tp, step).start()
    att_all[tp] = att[tp]

    each(half, n_ep, landed)
    each(0, local, lambda number: expert(number, half))
    hand_over(half)

    for step in range(1, n_tp):
        t_copy(lax.rem(tp - step + n_tp, n_tp), step).wait()
    total = None
    for source in range(n_tp):
        for head in range(heads):
            number = source * heads + head
            term = jnp.dot(
                att_all[source, head],
                mixer[number * head_dim : (number + 1) * head_dim, :],
                preferred_element_type=jnp.float32,
            )
            total = term if total is None else total + term
    mixed[...] = total.astype(jnp.bfloat16)

    each(0, half, lambda step: send_back(n_ep - 1 - step))

    def sent(slot):
        x_copy(outg.at[0], tp, slot).wait_send()
        c_copy(outg.at[0], tp, slot).wait_send()
        d_copy(outg.at[0], tp, slot).wait_send()
        far_copy(slot).wait_send()
        own_copy(slot).wait_send()
        y_copy(slot).wait_send()

    each(0, n_ep, sent)
    each(1, n_ep, lambda slot: a_copy(slot).wait_send())

    @pl.when(level + 1 < levels)
    def _():
        up_copy(kv, ep).wait_send()

    @pl.when(side == 0)
    def _():
        side_copy(kv, ep).wait_send()

    def spread_sent(k):
        source = ep - 2 * k
        side_copy(kv, source).wait_send()

        @pl.when(level + 1 < levels)
        def _():
            up_copy(kv, source).wait_send()

    each(1, level + 1, spread_sent)
    each(1, n_ep, lambda slot: r_copy(slot).wait())

    _, per, _ = back.shape
    found_rows = back[...].reshape(n_ep * per, width)
    summed = None
    top = slots_weights.shape[1] // 2
    for choice in range(top):
        lanes = lax.broadcasted_iota(jnp.int32, (mixed.shape[0], n_ep * per), 1)
        pick = jnp.where(
            lanes.astype(jnp.float32) == slots_weights[:, choice : choice + 1], 1.0, 0.0
        ).astype(jnp.bfloat16)
        found = jnp.dot(pick, found_rows, preferred_element_type=jnp.float32)
        term = found * slots_weights[:, top + choice : top + choice + 1]
        summed = term if summed is None else summed + term
    routed[...] = summed.astype(jnp.bfloat16)


def on_device(
    n_ep,
    n_tp,
    queries,
    keys,
    values,
    forget_cache,
    query_gain,
    key_gain,
    mixer_out,
    expert_input,
    norm_gain,
    routes,
    route_weights,
    w_gate,
    w_up,
    w_down,
):
    rows, head_dim = keys.shape
    heads = forget_cache.shape[0]
    ep = lax.axis_index("ep")
    local, width, ff = w_gate.shape
    experts = local * n_ep
    tokens = expert_input.shape[0]
    per = local * CAP
    part = rows // n_tp
    vmem = pl.BlockSpec(memory_space=pltpu.VMEM)
    anywhere = pl.BlockSpec(memory_space=pl.ANY)
    dma = pltpu.SemaphoreType.DMA

    normed_q = rms_scale(queries.reshape(rows, heads, head_dim), query_gain).astype(jnp.bfloat16)
    q = normed_q.transpose(1, 0, 2).reshape(heads * rows, head_dim)
    kv = jnp.concatenate([rms_scale(keys, key_gain).astype(jnp.bfloat16), values], axis=1)
    fq = lax.dynamic_slice_in_dim(forget_cache, ep * rows, rows, 1).reshape(heads * rows, 1)
    fk = forget_cache.reshape(heads, n_ep, rows).transpose(1, 0, 2)

    normed = rms_scale(expert_input, norm_gain).astype(jnp.bfloat16)
    names = jnp.arange(experts, dtype=jnp.int32)
    named = [(routes[:, k : k + 1] == names[None, :]) for k in range(routes.shape[1])]
    anyone = functools.reduce(jnp.logical_or, named).astype(jnp.bfloat16)
    at = jnp.arange(tokens, dtype=jnp.int32)
    earlier = (at[None, :] < at[:, None]).astype(jnp.bfloat16)
    prior = jnp.dot(earlier, anyone, preferred_element_type=jnp.float32)
    ranks = [jnp.sum(jnp.where(mine, prior, 0.0), axis=1).astype(jnp.int32) for mine in named]
    differ = (routes // local) ^ ep
    slot = jnp.zeros_like(routes)
    for number, weight in enumerate(weights_of(n_ep)):
        slot = slot + (1 << number) * (differ // weight % 2)
    base = slot * per + routes % local * CAP
    slots = jnp.stack([base[:, k] + rank for k, rank in enumerate(ranks)], axis=1)
    slots_weights = jnp.concatenate([slots.astype(jnp.float32), route_weights], axis=1)
    line = jnp.arange(experts * CAP, dtype=jnp.int32)[:, None]
    place = functools.reduce(
        jnp.logical_or, [line == slots[:, k][None, :] for k in range(slots.shape[1])]
    ).astype(jnp.bfloat16)
    outg = jnp.dot(place, normed, preferred_element_type=jnp.float32).astype(jnp.bfloat16)
    outg = outg.reshape(n_ep, per, width)

    buffer = pltpu.VMEM((n_ep, per, width), jnp.bfloat16)
    return pl.pallas_call(
        functools.partial(layer_kernel, n_ep, n_tp, heads),
        out_shape=(
            jax.ShapeDtypeStruct((part, width), jnp.bfloat16),
            jax.ShapeDtypeStruct((tokens, width), jnp.bfloat16),
        ),
        in_specs=[vmem] * 6 + [anywhere] * 4,
        out_specs=(vmem, vmem),
        scratch_shapes=[pltpu.VMEM(w_gate.shape, jnp.bfloat16)] * 3
        + [
            pltpu.VMEM(mixer_out.shape, jnp.bfloat16),
            pltpu.VMEM((n_ep, rows, 2 * head_dim), jnp.bfloat16),
            pltpu.VMEM((n_tp, heads, part, head_dim), jnp.bfloat16),
            pltpu.VMEM((n_tp, heads, part, head_dim), jnp.bfloat16),
            pltpu.VMEM((heads * rows, 1), jnp.float32),
            pltpu.VMEM((heads * rows, 1), jnp.float32),
            pltpu.VMEM((heads * rows, head_dim), jnp.float32),
            pltpu.VMEM((n_tp, n_ep, per, width), jnp.bfloat16),
            pltpu.VMEM((n_tp, n_ep, per, width), jnp.bfloat16),
        ]
        + [buffer] * 6
        + [dma((n_ep,))] * 19
        + [dma((n_tp,))] * 3
        + [dma],
        compiler_params=pltpu.CompilerParams(
            collective_id=0, has_side_effects=True, vmem_limit_bytes=VMEM_LIMIT
        ),
        name="layer",
    )(outg, kv, q, fq, fk, slots_weights, w_gate, w_up, w_down, mixer_out)


def solution(mesh):
    n_ep, n_tp = mesh.shape["ep"], mesh.shape["tp"]
    in_specs = (
        P("ep", "tp"),
        P("ep", "tp"),
        P("ep", "tp"),
        P("tp", None),
        P(),
        P(),
        P(),
        P(("ep", "tp"), None),
        P(),
        P(("ep", "tp"), None),
        P(("ep", "tp"), None),
        P("ep", None, "tp"),
        P("ep", None, "tp"),
        P("ep", None, "tp"),
    )
    out_specs = (P(("ep", "tp"), None), P(("ep", "tp"), None))
    return jax.shard_map(
        functools.partial(on_device, n_ep, n_tp),
        mesh=mesh,
        in_specs=in_specs,
        out_specs=out_specs,
        check_vma=False,
    )
```
